32 devices in a mesh: fs: 8 (over z, x), tp: 4 (over y, core).
Axes of the slice: x: 2, y: 2, z: 4, core: 2. Of those that a mesh axis runs over, the one named last changes fastest.
Arguments:
- h_saved: bfloat16 [16384, 2048], P('fs'), may hold values from -6 to 6
- conv_cotan: bfloat16 [16384, 2560], P('fs', 'tp'), may hold values from -64 to 64
- lru_out: bfloat16 [16384, 2560], P('fs', 'tp'), may hold values from -64 to 64
- out_cotan: bfloat16 [16384, 2048], P('fs'), may hold values from -6 to 6
- basis_in: bfloat16 [2048, 256], P('fs'), may hold values from -1.41421356 to 1.41421356
- basis_out: bfloat16 [2048, 256], P('fs'), may hold values from -1.41421356 to 1.41421356
- weight_in: float32 [2048, 2560], P('fs', 'tp'), may hold values from -0.125 to 0.125
- weight_out: float32 [2560, 2048], P('tp', 'fs'), may hold values from -0.125 to 0.125
- first_in: float32 [256, 2560], P('fs', 'tp'), may hold values from -6 to 6
- second_in: float32 [256, 2560], P('fs', 'tp'), may hold values from 0.05 to 2
- first_out: float32 [256, 2560], P('fs', 'tp'), may hold values from -6 to 6
- second_out: float32 [256, 2560], P('fs', 'tp'), may hold values from 0.05 to 2
Outputs:
- step_in: float32 [2048, 2560], P('fs', 'tp')
- new_weight_in: float32 [2048, 2560], P('fs', 'tp')
- copy_in: bfloat16 [2048, 2560], P(None, 'tp')
- new_first_in: float32 [256, 2560], P('fs', 'tp')
- new_second_in: float32 [256, 2560], P('fs', 'tp')
- step_out: float32 [2560, 2048], P('tp', 'fs')
- new_weight_out: float32 [2560, 2048], P('tp', 'fs')
- copy_out: bfloat16 [2560, 2048], P('tp')
- new_first_out: float32 [256, 2560], P('fs', 'tp')
- new_second_out: float32 [256, 2560], P('fs', 'tp')
The draws below stay inside these ranges and needn't reach their ends.
All inputs are finite; a program needn't handle non-finite values.
Results may differ from the reference program's by a relative error of at most 0.0046.
Values may be sent and summed in bfloat16 or wider, within the bound.
A program may use at most 128 MiB of HBM per device.

```python
import math
import jax
import jax.numpy as jnp
from jax import lax

D_MODEL = 2048
D_RNN = 2560
RANK = 256
TOKENS = 16384


def scaled_field(key, count, columns):
    keyone, keytwo = jax.random.split(key, 2)
    place = jnp.arange(columns, dtype=jnp.float32) / max(columns - 1, 1)
    rough = jnp.exp(jax.random.uniform(keytwo, (columns,), jnp.float32, math.log(0.5), math.log(2.0)))
    column_scale = jnp.exp(math.log(3.0) * place) * rough
    values = jnp.clip(jax.random.normal(keyone, (count, columns), jnp.float32), -6.0, 6.0)
    return values * column_scale


def draw_conv_cotan(key, part):
    return scaled_field(jax.random.fold_in(key, 11), TOKENS, D_RNN).astype(jnp.bfloat16)


def draw_lru_out(key, part):
    return scaled_field(jax.random.fold_in(key, 12), TOKENS, D_RNN).astype(jnp.bfloat16)


def draw_basis_in(key, part):
    return (scaled_field(jax.random.fold_in(key, 13), D_MODEL, RANK) / math.sqrt(D_MODEL)).astype(jnp.bfloat16)


def draw_basis_out(key, part):
    return (scaled_field(jax.random.fold_in(key, 14), D_MODEL, RANK) / math.sqrt(D_MODEL)).astype(jnp.bfloat16)


def block_scale(rng, dims, pieces, smallest, largest):
    level = 1.0
    for axis_at, blocks in pieces:
        steps = jax.random.uniform(jax.random.fold_in(jax.random.fold_in(rng, 6), axis_at), (blocks,), jnp.float32, smallest / len(pieces), largest / len(pieces))
        level = level * jnp.repeat(jnp.exp(steps), dims[axis_at] // blocks).reshape((-1,) + (1,) * (len(dims) - 1 - axis_at))
    return level


def scatter_about(stream_key, dims, width, most, shards=(), kind=jnp.bfloat16):
    loudness = block_scale(stream_key, dims, shards, -0.22, 0.18) if shards else 1.0
    values = jax.random.normal(stream_key, dims, jnp.float32) * width * loudness
    return jnp.minimum(jnp.maximum(values, -most), most).astype(kind)


def setup_inputs(seed: int = 0) -> dict:
    key_list = jax.random.split(jax.random.key(seed), 13)
    return {
        "h_saved": scatter_about(key_list[0], (TOKENS, D_MODEL), 1.0, 6.0, ((0, 8),)),
        "conv_cotan": draw_conv_cotan(jax.random.fold_in(key_list[12], 71), 0),
        "lru_out": draw_lru_out(jax.random.fold_in(key_list[12], 71), 0),
        "out_cotan": scatter_about(key_list[3], (TOKENS, D_MODEL), 1.0, 6.0, ((0, 8),)),
        "basis_in": draw_basis_in(jax.random.fold_in(key_list[12], 71), 0),
        "basis_out": draw_basis_out(jax.random.fold_in(key_list[12], 71), 0),
        "weight_in": scatter_about(key_list[6], (D_MODEL, D_RNN), D_MODEL ** -0.5, 0.125, ((0, 8), (1, 4)), jnp.float32),
        "weight_out": scatter_about(key_list[7], (D_RNN, D_MODEL), D_RNN ** -0.5, 0.125, ((0, 4), (1, 8)), jnp.float32),
        "first_in": scatter_about(key_list[8], (RANK, D_RNN), 1.0, 6.0, ((0, 8), (1, 4)), jnp.float32),
        "second_in": jnp.clip(jnp.exp(math.log(2.0) - 3.6888794 * jax.random.uniform(key_list[9], (RANK, D_RNN), jnp.float32) ** block_scale(key_list[9], (RANK, D_RNN), ((0, 8), (1, 4)), -0.2, 0.2)), 0.05, 2.0),
        "first_out": scatter_about(key_list[10], (RANK, D_RNN), 1.0, 6.0, ((0, 8), (1, 4)), jnp.float32),
        "second_out": jnp.clip(jnp.exp(math.log(2.0) - 3.6888794 * jax.random.uniform(key_list[11], (RANK, D_RNN), jnp.float32) ** block_scale(key_list[11], (RANK, D_RNN), ((0, 8), (1, 4)), -0.2, 0.2)), 0.05, 2.0),
    }


def exact_dot(left, right):
    return jnp.dot(left.astype(jnp.float32), right.astype(jnp.float32), precision=lax.Precision.HIGHEST)

def projected(inputs, cotan, basis):
    grad = exact_dot(inputs.T, cotan)
    return jnp.dot(basis.astype(jnp.float32).T, grad, precision=lax.Precision.HIGHEST)

def moments(proj, factor, first, second):
    scaled = factor * proj
    first_new = 0.8 * first + 0.2 * scaled
    second_new = 0.9 * second + 0.1 * scaled * scaled
    direction = (first_new / (jnp.sqrt(second_new) + 1e-08)).astype(jnp.bfloat16)
    return (first_new, second_new, direction)

def reference(h_saved, conv_cotan, lru_out, out_cotan, basis_in, basis_out, weight_in, weight_out, first_in, second_in, first_out, second_out):
    proj_in = projected(h_saved, conv_cotan, basis_in)
    proj_out = projected(out_cotan, lru_out, basis_out)
    total = jnp.sum(proj_in * proj_in) + jnp.sum(proj_out * proj_out)
    factor = math.sqrt(2.0 * RANK * D_RNN) * lax.rsqrt(total + 1e-06)
    first_a, second_a, dir_in = moments(proj_in, factor, first_in, second_in)
    first_b, second_b, dir_out = moments(proj_out, factor, first_out, second_out)
    step_in = exact_dot(basis_in, dir_in)
    step_out = exact_dot(basis_out, dir_out).T
    new_in = weight_in - 0.02 * step_in
    new_out = weight_out - 0.02 * step_out
    return (step_in, new_in, new_in.astype(jnp.bfloat16), first_a, second_a, step_out, new_out, new_out.astype(jnp.bfloat16), first_b, second_b)
```

```python
import functools
import math

import jax
import jax.numpy as jnp
from jax import lax
from jax.experimental import pallas as pl
from jax.experimental.pallas import tpu as pltpu
from jax.sharding import PartitionSpec as P

MESH = pl.DeviceIdType.MESH
VMEM_LIMIT = 60 * 1024 * 1024


def nt_dot(left, right):
    return lax.dot_general(left, right, (((1,), (1,)), ((), ())), preferred_element_type=jnp.float32)


def exchange(
    dims,
    h_hbm,
    cc_hbm,
    oc_hbm,
    lo_hbm,
    basis_in,
    basis_out,
    w_in,
    w_out,
    m_in,
    v_in,
    m_out,
    v_out,
    ball,
    win_all,
    wout_all,
    dall,
    nm_in,
    nv_in,
    nm_out,
    nv_out,
    h_buf,
    c_buf,
    acc,
    part,
    part_in,
    tot,
    tot_in,
    in_sem,
    ss,
    rs,
    cs,
    cr,
    ps,
    pr,
    ts,
    tr,
):
    F, T, Z, X, scale = dims
    f = lax.axis_index("fs")
    t = lax.axis_index("tp")
    z, x = f // X, f % X
    core = t % 2
    mate = t + 1 - 2 * core
    tokens, chunk = h_buf.shape[1], h_buf.shape[1] // in_sem.shape[1]
    chunks = in_sem.shape[1]
    rr = m_in.shape[0]

    def fetch(which, i):
        rows = pl.ds(i * chunk, chunk)
        h_src, c_src = ((h_hbm, cc_hbm), (oc_hbm, lo_hbm))[which]
        return (
            pltpu.make_async_copy(h_src.at[rows], h_buf.at[which, rows], in_sem.at[which, i, 0]),
            pltpu.make_async_copy(c_src.at[rows], c_buf.at[which, rows], in_sem.at[which, i, 1]),
        )

    for which in range(2):
        for i in range(chunks):
            for copy in fetch(which, i):
                copy.start()

    barrier = pltpu.get_barrier_semaphore()

    def greet(n, carry):
        pl.semaphore_signal(
            barrier, inc=1, device_id=((f + n // T) % F, (t + n % T) % T), device_id_type=MESH
        )
        return carry

    lax.fori_loop(1, F * T, greet, 0)
    for which, basis in enumerate((basis_in, basis_out)):
        ball[which, f] = basis[...]
    win_all[f] = w_in[...].astype(jnp.bfloat16)
    wout_all[f] = w_out[...].astype(jnp.bfloat16)
    pl.semaphore_wait(barrier, F * T - 1)

    def source(k, j):
        return ((z + Z - k) % Z) * X + (x + X - j) % X

    half = basis_in.shape[0] // 2
    q_in, q_out = w_in.shape[0] // 2, w_out.shape[0] // 2

    def place(item, s, core):
        if item < 2:
            return ball.at[item, s, pl.ds(pl.multiple_of(core * half, half), half)]
        if item < 4:
            return win_all.at[s, pl.ds((item - 2) * q_in, q_in)]
        if item < 6:
            return wout_all.at[s, pl.ds((item - 4) * q_out, q_out)]
        return dall.at[item - 6, s]

    def own(item):
        if item < 2:
            return (basis_in, basis_out)[item].at[pl.ds(pl.multiple_of(core * half, half), half)]
        return place(item, f, core)

    def along_z(item, k, src=None):
        at = place(item, f, core)
        return pltpu.make_async_remote_copy(
            src_ref=at if src is None else src,
            dst_ref=at,
            send_sem=ss.at[item, k, 0],
            recv_sem=rs.at[item, k, 0],
            device_id=(((z + k) % Z) * X + x, t),
            device_id_type=MESH,
        )

    def along_x(item, k, j, src=None):
        at = place(item, source(k, 0), core)
        return pltpu.make_async_remote_copy(
            src_ref=at if src is None else src,
            dst_ref=at,
            send_sem=ss.at[item, k, j],
            recv_sem=rs.at[item, k, j],
            device_id=(z * X + (x + j) % X, t),
            device_id_type=MESH,
        )

    def across(item, k, j, side=None):
        at = place(item, source(k, j), core if side is None else side)
        return pltpu.make_async_remote_copy(
            src_ref=at,
            dst_ref=at,
            send_sem=cs.at[item, k, j],
            recv_sem=cr.at[item, k, j],
            device_id=(f, mate),
            device_id_type=MESH,
        )

    def arrived(item, k, j):
        at = place(item, source(k, j), core)
        pltpu.make_async_remote_copy(
            src_ref=at,
            dst_ref=at,
            send_sem=ss.at[item, k, j],
            recv_sem=rs.at[item, k, j],
            device_id=((f + 1) % F, t),
            device_id_type=MESH,
        ).wait_recv()

    def begin(item):
        src = own(item)
        for k in range(1, Z):
            along_z(item, k, src).start()
        for j in range(1, X):
            along_x(item, 0, j, src).start()

    def forward(item):
        for k in range(1, Z):
            arrived(item, k, 0)
            for j in range(1, X):
                along_x(item, k, j).start()
            if item < 2:
                across(item, k, 0).start()

    def finish(item):
        for k in range(Z):
            for j in range(1, X):
                arrived(item, k, j)
                if item < 2:
                    across(item, k, j).start()
        if item < 2:
            for k in range(Z):
                for j in range(X):
                    if k or j:
                        across(item, k, j, 1 - core).wait_recv()

    def drain(item):
        for k in range(Z):
            for j in range(X):
                if j:
                    along_x(item, k, j).wait_send()
                elif k:
                    along_z(item, k).wait_send()
                if item < 2 and (k or j):
                    across(item, k, j).wait_send()

    def project(which):
        acc[which] = jnp.zeros(acc.shape[1:], jnp.float32)

        def step(i, carry):
            for copy in fetch(which, i):
                copy.wait()
            rows = pl.ds(pl.multiple_of(i * chunk, chunk), chunk)
            whole = ball[which].reshape(h_buf.shape[2], -1)
            reduced = jnp.dot(h_buf[which, rows], whole, preferred_element_type=jnp.float32)
            turned = reduced.T
            upper = turned.astype(jnp.bfloat16)
            lower = (turned - upper.astype(jnp.float32)).astype(jnp.bfloat16)
            block = c_buf[which, rows]
            acc[which] += jnp.dot(upper, block, preferred_element_type=jnp.float32) + jnp.dot(
                lower, block, preferred_element_type=jnp.float32
            )
            return carry

        lax.fori_loop(0, chunks, step, 0)
        part[which] = acc[which].astype(jnp.bfloat16).reshape(part.shape[1:])

    def scatter(which, d):
        peer = (f + d) % F
        return pltpu.make_async_remote_copy(
            src_ref=part.at[which, peer],
            dst_ref=part_in.at[which, d],
            send_sem=ps.at[which, d],
            recv_sem=pr.at[which, d],
            device_id=(peer, t),
            device_id_type=MESH,
        )

    def share(n):
        return pltpu.make_async_remote_copy(
            src_ref=tot,
            dst_ref=tot_in.at[n],
            send_sem=ts.at[n],
            recv_sem=tr.at[n],
            device_id=((f + n // T) % F, (t + n % T) % T),
            device_id_type=MESH,
        )

    begin(0)
    begin(1)
    forward(0)
    forward(1)
    begin(2)
    finish(0)
    project(0)
    for d in range(1, F):
        scatter(0, d).start()
    finish(1)
    project(1)
    for d in range(1, F):
        scatter(1, d).start()
    forward(2)
    begin(3)
    projs = []
    square = jnp.zeros((1, 1), jnp.float32)
    for which in range(2):
        value = acc[which, pl.ds(pl.multiple_of(f * rr, rr), rr)]
        for d in range(1, F):
            scatter(which, d).wait_recv()
            value = value + part_in[which, d].astype(jnp.float32)
        projs.append(value)
        square = square + jnp.sum(value * value, axis=(0, 1), keepdims=True)
    tot[...] = jnp.broadcast_to(square, tot.shape)
    tot_in[0] = tot[...]

    def share_start(n, carry):
        share(n).start()
        return carry

    def share_wait(n, carry):
        share(n).wait()
        return carry

    lax.fori_loop(1, F * T, share_start, 0)
    lax.fori_loop(1, F * T, share_wait, 0)
    total = jnp.sum(tot_in[...], axis=0)
    factor = (scale * lax.rsqrt(total + 1e-06))[0:1, 0:1]
    for which, (first, second, first_to, second_to) in enumerate(
        ((m_in, v_in, nm_in, nv_in), (m_out, v_out, nm_out, nv_out))
    ):
        scaled = factor * projs[which]
        first_new = 0.8 * first[...] + 0.2 * scaled
        second_new = 0.9 * second[...] + 0.1 * scaled * scaled
        first_to[...] = first_new
        second_to[...] = second_new
        dall[which, f] = (first_new / (jnp.sqrt(second_new) + 1e-08)).astype(jnp.bfloat16)
    begin(6)
    begin(7)
    begin(4)
    begin(5)
    forward(3)
    forward(6)
    forward(7)
    forward(4)
    forward(5)
    for item in (2, 3, 6, 7, 4, 5):
        finish(item)
    for item in range(8):
        drain(item)
    for which in range(2):
        for d in range(1, F):
            scatter(which, d).wait_send()


def apply_step(
    basis_in, basis_out, w_in, w_out, nm_in, nv_in, nm_out, nv_out, b_in, b_out, win, wout, dirs,
    step_in, new_in, copy_in, o_m_in, o_v_in, step_out, new_out, copy_out, o_m_out, o_v_out, turned,
):
    direction = dirs[0].reshape(-1, dirs.shape[3])

    @pl.when(pl.program_id(0) == 0)
    def _():
        other = dirs[1].reshape(-1, dirs.shape[3])
        turned[...] = other.astype(jnp.float32).T.astype(jnp.bfloat16)
        for source, target in ((nm_in, o_m_in), (nv_in, o_v_in), (nm_out, o_m_out), (nv_out, o_v_out)):
            target[...] = source[...]
        step = jnp.dot(basis_in[...], direction, preferred_element_type=jnp.float32)
        step_in[...] = step
        new_in[...] = w_in[...] - 0.02 * step
        step = nt_dot(turned[...], basis_out[...])
        step_out[...] = step
        new_out[...] = w_out[...] - 0.02 * step

    step = jnp.dot(b_in[0, 0], direction, preferred_element_type=jnp.float32)
    copy_in[...] = (win[0].astype(jnp.float32) - 0.02 * step).astype(jnp.bfloat16)
    step = nt_dot(turned[...], b_out[0, 0])
    copy_out[...] = (wout[0].astype(jnp.float32) - 0.02 * step).astype(jnp.bfloat16)


def shards(mesh, h, cc, lo, oc, basis_in, basis_out, w_in, w_out, m_in, v_in, m_out, v_out):
    F, T = mesh.shape["fs"], mesh.shape["tp"]
    Z = next(n for n in range(1, F + 1) if F % n == 0 and n * n >= F)
    X = F // Z
    tokens, model = h.shape
    cols = cc.shape[1]
    rows, rank = basis_in.shape
    rr = m_in.shape[0]
    scale = math.sqrt(2.0 * rank * cols * T)
    chunks = max(1, tokens // 512)
    bf, f32 = jnp.bfloat16, jnp.float32
    hbm = pl.BlockSpec(memory_space=pl.ANY)
    vmem = pl.BlockSpec(memory_space=pltpu.VMEM)
    moment = jax.ShapeDtypeStruct(m_in.shape, f32)
    dma = pltpu.SemaphoreType.DMA
    ball, win_all, wout_all, dall, *moments = pl.pallas_call(
        functools.partial(exchange, (F, T, Z, X, scale)),
        out_shape=(
            jax.ShapeDtypeStruct((2, F, rows, rank), bf),
            jax.ShapeDtypeStruct((F,) + w_in.shape, bf),
            jax.ShapeDtypeStruct((F,) + w_out.shape, bf),
            jax.ShapeDtypeStruct((2, F, rr, cols), bf),
            moment,
            moment,
            moment,
            moment,
        ),
        in_specs=[hbm] * 4 + [vmem] * 8,
        out_specs=(vmem,) * 8,
        scratch_shapes=[
            pltpu.VMEM((2, tokens, model), bf),
            pltpu.VMEM((2, tokens, cols), bf),
            pltpu.VMEM((2, rank, cols), f32),
            pltpu.VMEM((2, F, rr, cols), bf),
            pltpu.VMEM((2, F, rr, cols), bf),
            pltpu.VMEM((8, 128), f32),
            pltpu.VMEM((F * T, 8, 128), f32),
            dma((2, chunks, 2)),
            dma((8, Z, X)),
            dma((8, Z, X)),
            dma((2, Z, X)),
            dma((2, Z, X)),
            dma((2, F)),
            dma((2, F)),
            dma((F * T,)),
            dma((F * T,)),
        ],
        compiler_params=pltpu.CompilerParams(
            collective_id=0, has_side_effects=True, vmem_limit_bytes=VMEM_LIMIT
        ),
        name="exchange",
    )(h, cc, oc, lo, basis_in, basis_out, w_in, w_out, m_in, v_in, m_out, v_out)

    def fixed(array):
        return pl.BlockSpec(array.shape, lambda i, n=array.ndim: (0,) * n)

    keep = (basis_in, basis_out, w_in, w_out, *moments)
    outs = (
        (w_in.shape, f32, None),
        (w_in.shape, f32, None),
        ((model, cols), bf, pl.BlockSpec(w_in.shape, lambda i: (i, 0))),
        (m_in.shape, f32, None),
        (m_in.shape, f32, None),
        (w_out.shape, f32, None),
        (w_out.shape, f32, None),
        ((cols, model), bf, pl.BlockSpec(w_out.shape, lambda i: (0, i))),
        (m_in.shape, f32, None),
        (m_in.shape, f32, None),
    )
    return pl.pallas_call(
        apply_step,
        grid=(F,),
        out_shape=tuple(jax.ShapeDtypeStruct(shape, kind) for shape, kind, _ in outs),
        in_specs=[fixed(a) for a in keep]
        + [
            pl.BlockSpec((1, 1, rows, rank), lambda i: (0, i, 0, 0)),
            pl.BlockSpec((1, 1, rows, rank), lambda i: (1, i, 0, 0)),
            pl.BlockSpec((1,) + w_in.shape, lambda i: (i, 0, 0)),
            pl.BlockSpec((1,) + w_out.shape, lambda i: (i, 0, 0)),
            fixed(dall),
        ],
        out_specs=tuple(
            spec or pl.BlockSpec(shape, lambda i, n=len(shape): (0,) * n) for shape, _, spec in outs
        ),
        scratch_shapes=[pltpu.VMEM((cols, rank), bf)],
        compiler_params=pltpu.CompilerParams(vmem_limit_bytes=VMEM_LIMIT),
        name="apply_step",
    )(*keep, ball, ball, win_all, wout_all, dall)


def solution(mesh):
    split, both = P("fs", None), P("fs", "tp")
    return jax.shard_map(
        functools.partial(shards, mesh),
        mesh=mesh,
        in_specs=(split, both, both, split, split, split, both, P("tp", "fs"), both, both, both, both),
        out_specs=(both, both, P(None, "tp"), both, both, P("tp", "fs"), P("tp", "fs"), P("tp", None), both, both),
        check_vma=False,
    )
```

```python
import functools
import math

import jax
import jax.numpy as jnp
from jax import lax
from jax.experimental import pallas as pl
from jax.experimental.pallas import tpu as pltpu
from jax.sharding import PartitionSpec as P

MESH = pl.DeviceIdType.MESH
VMEM_LIMIT = 60 * 1024 * 1024


def nt_dot(left, right):
    return lax.dot_general(left, right, (((1,), (1,)), ((), ())), preferred_element_type=jnp.float32)


def exchange(
    dims,
    h_hbm,
    cc_hbm,
    oc_hbm,
    lo_hbm,
    basis_in,
    basis_out,
    w_in,
    w_out,
    m_in,
    v_in,
    m_out,
    v_out,
    ball,
    win_all,
    wout_all,
    dall,
    nm_in,
    nv_in,
    nm_out,
    nv_out,
    h_buf,
    c_buf,
    acc,
    part,
    part_in,
    tot,
    tot_two,
    tot_in,
    in_sem,
    ss,
    rs,
    cs,
    cr,
    ps,
    pr,
    ts,
    tr,
):
    F, T, Z, X, scale = dims
    f = lax.axis_index("fs")
    t = lax.axis_index("tp")
    z, x = f // X, f % X
    core = t % 2
    mate = t + 1 - 2 * core
    tokens, chunk = h_buf.shape[1], h_buf.shape[1] // in_sem.shape[1]
    chunks = in_sem.shape[1]
    rr = m_in.shape[0]

    def fetch(which, i):
        rows = pl.ds(i * chunk, chunk)
        h_src, c_src = ((h_hbm, cc_hbm), (oc_hbm, lo_hbm))[which]
        return (
            pltpu.make_async_copy(h_src.at[rows], h_buf.at[which, rows], in_sem.at[which, i, 0]),
            pltpu.make_async_copy(c_src.at[rows], c_buf.at[which, rows], in_sem.at[which, i, 1]),
        )

    for which in range(2):
        for i in range(chunks):
            for copy in fetch(which, i):
                copy.start()

    barrier = pltpu.get_barrier_semaphore()

    def greet(n, carry):
        pl.semaphore_signal(
            barrier, inc=1, device_id=((f + n // T) % F, (t + n % T) % T), device_id_type=MESH
        )
        return carry

    lax.fori_loop(1, F * T, greet, 0)
    for which, basis in enumerate((basis_in, basis_out)):
        ball[which, f] = basis[...]
    win_all[f] = w_in[...].astype(jnp.bfloat16)
    wout_all[f] = w_out[...].astype(jnp.bfloat16)
    pl.semaphore_wait(barrier, F * T - 1)

    def source(k, j):
        return ((z + Z - k) % Z) * X + (x + X - j) % X

    half = basis_in.shape[0] // 2
    q_in, q_out = w_in.shape[0] // 2, w_out.shape[0] // 2

    def place(item, s, core):
        if item < 2:
            return ball.at[item, s, pl.ds(pl.multiple_of(core * half, half), half)]
        if item < 4:
            return win_all.at[s, pl.ds((item - 2) * q_in, q_in)]
        if item < 6:
            return wout_all.at[s, pl.ds((item - 4) * q_out, q_out)]
        return dall.at[item - 6, s]

    def own(item):
        if item < 2:
            return (basis_in, basis_out)[item].at[pl.ds(pl.multiple_of(core * half, half), half)]
        return place(item, f, core)

    def along_z(item, k, src=None):
        at = place(item, f, core)
        return pltpu.make_async_remote_copy(
            src_ref=at if src is None else src,
            dst_ref=at,
            send_sem=ss.at[item, k, 0],
            recv_sem=rs.at[item, k, 0],
            device_id=(((z + k) % Z) * X + x, t),
            device_id_type=MESH,
        )

    def along_x(item, k, j, src=None):
        at = place(item, source(k, 0), core)
        return pltpu.make_async_remote_copy(
            src_ref=at if src is None else src,
            dst_ref=at,
            send_sem=ss.at[item, k, j],
            recv_sem=rs.at[item, k, j],
            device_id=(z * X + (x + j) % X, t),
            device_id_type=MESH,
        )

    def across(item, k, j, side=None):
        at = place(item, source(k, j), core if side is None else side)
        return pltpu.make_async_remote_copy(
            src_ref=at,
            dst_ref=at,
            send_sem=cs.at[item, k, j],
            recv_sem=cr.at[item, k, j],
            device_id=(f, mate),
            device_id_type=MESH,
        )

    def arrived(item, k, j):
        at = place(item, source(k, j), core)
        pltpu.make_async_remote_copy(
            src_ref=at,
            dst_ref=at,
            send_sem=ss.at[item, k, j],
            recv_sem=rs.at[item, k, j],
            device_id=((f + 1) % F, t),
            device_id_type=MESH,
        ).wait_recv()

    def begin(item):
        src = own(item)
        for k in range(1, Z):
            along_z(item, k, src).start()
        for j in range(1, X):
            along_x(item, 0, j, src).start()

    def forward(item):
        for k in range(1, Z):
            arrived(item, k, 0)
            for j in range(1, X):
                along_x(item, k, j).start()
            if item < 2:
                across(item, k, 0).start()

    def finish(item):
        for k in range(Z):
            for j in range(1, X):
                arrived(item, k, j)
                if item < 2:
                    across(item, k, j).start()
        if item < 2:
            for k in range(Z):
                for j in range(X):
                    if k or j:
                        across(item, k, j, 1 - core).wait_recv()

    def drain(item):
        for k in range(Z):
            for j in range(X):
                if j:
                    along_x(item, k, j).wait_send()
                elif k:
                    along_z(item, k).wait_send()
                if item < 2 and (k or j):
                    across(item, k, j).wait_send()

    def project(which):
        acc[which] = jnp.zeros(acc.shape[1:], jnp.float32)

        def step(i, carry):
            for copy in fetch(which, i):
                copy.wait()
            rows = pl.ds(pl.multiple_of(i * chunk, chunk), chunk)
            whole = ball[which].reshape(h_buf.shape[2], -1)
            reduced = jnp.dot(h_buf[which, rows], whole, preferred_element_type=jnp.float32)
            turned = reduced.T
            upper = turned.astype(jnp.bfloat16)
            lower = (turned - upper.astype(jnp.float32)).astype(jnp.bfloat16)
            block = c_buf[which, rows]
            acc[which] += jnp.dot(upper, block, preferred_element_type=jnp.float32) + jnp.dot(
                lower, block, preferred_element_type=jnp.float32
            )
            return carry

        lax.fori_loop(0, chunks, step, 0)
        part[which] = acc[which].astype(jnp.bfloat16).reshape(part.shape[1:])

    def scatter(which, d):
        peer = (f + d) % F
        return pltpu.make_async_remote_copy(
            src_ref=part.at[which, peer],
            dst_ref=part_in.at[which, d],
            send_sem=ps.at[which, d],
            recv_sem=pr.at[which, d],
            device_id=(peer, t),
            device_id_type=MESH,
        )

    def share(n):
        return pltpu.make_async_remote_copy(
            src_ref=tot,
            dst_ref=tot_in.at[n],
            send_sem=ts.at[n],
            recv_sem=tr.at[n],
            device_id=(f, (t + n) % T),
            device_id_type=MESH,
        )

    def share_on(d):
        return pltpu.make_async_remote_copy(
            src_ref=tot_two,
            dst_ref=tot_in.at[T + d],
            send_sem=ts.at[T + d],
            recv_sem=tr.at[T + d],
            device_id=((f + d) % F, t),
            device_id_type=MESH,
        )

    begin(0)
    begin(1)
    forward(0)
    forward(1)
    begin(2)
    finish(0)
    project(0)
    for d in range(1, F):
        scatter(0, d).start()
    finish(1)
    project(1)
    for d in range(1, F):
        scatter(1, d).start()
    forward(2)
    begin(3)
    projs = []
    square = jnp.zeros((1, 1), jnp.float32)
    for which in range(2):
        value = acc[which, pl.ds(pl.multiple_of(f * rr, rr), rr)]
        for d in range(1, F):
            scatter(which, d).wait_recv()
            value = value + part_in[which, d].astype(jnp.float32)
        projs.append(value)
        square = square + jnp.sum(value * value, axis=(0, 1), keepdims=True)
    tot[...] = jnp.broadcast_to(square, tot.shape)
    tot_in[0] = tot[...]

    for n in range(1, T):
        share(n).start()
    for n in range(1, T):
        share(n).wait()
    tot_two[...] = jnp.sum(tot_in[:T], axis=0)
    tot_in[T] = tot_two[...]
    for d in range(1, F):
        share_on(d).start()
    for d in range(1, F):
        share_on(d).wait()
    total = jnp.sum(tot_in[T:], axis=0)
    factor = (scale * lax.rsqrt(total + 1e-06))[0:1, 0:1]
    for which, (first, second, first_to, second_to) in enumerate(
        ((m_in, v_in, nm_in, nv_in), (m_out, v_out, nm_out, nv_out))
    ):
        scaled = factor * projs[which]
        first_new = 0.8 * first[...] + 0.2 * scaled
        second_new = 0.9 * second[...] + 0.1 * scaled * scaled
        first_to[...] = first_new
        second_to[...] = second_new
        dall[which, f] = (first_new / (jnp.sqrt(second_new) + 1e-08)).astype(jnp.bfloat16)
    begin(6)
    begin(7)
    begin(4)
    begin(5)
    forward(3)
    forward(6)
    forward(7)
    forward(4)
    forward(5)
    for item in (2, 3, 6, 7, 4, 5):
        finish(item)
    for item in range(8):
        drain(item)
    for which in range(2):
        for d in range(1, F):
            scatter(which, d).wait_send()


def apply_step(
    basis_in, basis_out, w_in, w_out, nm_in, nv_in, nm_out, nv_out, b_in, b_out, win, wout, dirs,
    step_in, new_in, copy_in, o_m_in, o_v_in, step_out, new_out, copy_out, o_m_out, o_v_out, turned,
):
    direction = dirs[0].reshape(-1, dirs.shape[3])

    @pl.when(pl.program_id(0) == 0)
    def _():
        other = dirs[1].reshape(-1, dirs.shape[3])
        turned[...] = other.astype(jnp.float32).T.astype(jnp.bfloat16)
        for source, target in ((nm_in, o_m_in), (nv_in, o_v_in), (nm_out, o_m_out), (nv_out, o_v_out)):
            target[...] = source[...]
        step = jnp.dot(basis_in[...], direction, preferred_element_type=jnp.float32)
        step_in[...] = step
        new_in[...] = w_in[...] - 0.02 * step
        step = nt_dot(turned[...], basis_out[...])
        step_out[...] = step
        new_out[...] = w_out[...] - 0.02 * step

    step = jnp.dot(b_in[0, 0], direction, preferred_element_type=jnp.float32)
    copy_in[...] = (win[0].astype(jnp.float32) - 0.02 * step).astype(jnp.bfloat16)
    step = nt_dot(turned[...], b_out[0, 0])
    copy_out[...] = (wout[0].astype(jnp.float32) - 0.02 * step).astype(jnp.bfloat16)


def shards(mesh, h, cc, lo, oc, basis_in, basis_out, w_in, w_out, m_in, v_in, m_out, v_out):
    F, T = mesh.shape["fs"], mesh.shape["tp"]
    Z = next(n for n in range(1, F + 1) if F % n == 0 and n * n >= F)
    X = F // Z
    tokens, model = h.shape
    cols = cc.shape[1]
    rows, rank = basis_in.shape
    rr = m_in.shape[0]
    scale = math.sqrt(2.0 * rank * cols * T)
    chunks = max(1, tokens // 512)
    bf, f32 = jnp.bfloat16, jnp.float32
    hbm = pl.BlockSpec(memory_space=pl.ANY)
    vmem = pl.BlockSpec(memory_space=pltpu.VMEM)
    moment = jax.ShapeDtypeStruct(m_in.shape, f32)
    dma = pltpu.SemaphoreType.DMA
    ball, win_all, wout_all, dall, *moments = pl.pallas_call(
        functools.partial(exchange, (F, T, Z, X, scale)),
        out_shape=(
            jax.ShapeDtypeStruct((2, F, rows, rank), bf),
            jax.ShapeDtypeStruct((F,) + w_in.shape, bf),
            jax.ShapeDtypeStruct((F,) + w_out.shape, bf),
            jax.ShapeDtypeStruct((2, F, rr, cols), bf),
            moment,
            moment,
            moment,
            moment,
        ),
        in_specs=[hbm] * 4 + [vmem] * 8,
        out_specs=(vmem,) * 8,
        scratch_shapes=[
            pltpu.VMEM((2, tokens, model), bf),
            pltpu.VMEM((2, tokens, cols), bf),
            pltpu.VMEM((2, rank, cols), f32),
            pltpu.VMEM((2, F, rr, cols), bf),
            pltpu.VMEM((2, F, rr, cols), bf),
            pltpu.VMEM((8, 128), f32),
            pltpu.VMEM((8, 128), f32),
            pltpu.VMEM((T + F, 8, 128), f32),
            dma((2, chunks, 2)),
            dma((8, Z, X)),
            dma((8, Z, X)),
            dma((2, Z, X)),
            dma((2, Z, X)),
            dma((2, F)),
            dma((2, F)),
            dma((T + F,)),
            dma((T + F,)),
        ],
        compiler_params=pltpu.CompilerParams(
            collective_id=0, has_side_effects=True, vmem_limit_bytes=VMEM_LIMIT
        ),
        name="exchange",
    )(h, cc, oc, lo, basis_in, basis_out, w_in, w_out, m_in, v_in, m_out, v_out)

    def fixed(array):
        return pl.BlockSpec(array.shape, lambda i, n=array.ndim: (0,) * n)

    keep = (basis_in, basis_out, w_in, w_out, *moments)
    outs = (
        (w_in.shape, f32, None),
        (w_in.shape, f32, None),
        ((model, cols), bf, pl.BlockSpec(w_in.shape, lambda i: (i, 0))),
        (m_in.shape, f32, None),
        (m_in.shape, f32, None),
        (w_out.shape, f32, None),
        (w_out.shape, f32, None),
        ((cols, model), bf, pl.BlockSpec(w_out.shape, lambda i: (0, i))),
        (m_in.shape, f32, None),
        (m_in.shape, f32, None),
    )
    return pl.pallas_call(
        apply_step,
        grid=(F,),
        out_shape=tuple(jax.ShapeDtypeStruct(shape, kind) for shape, kind, _ in outs),
        in_specs=[fixed(a) for a in keep]
        + [
            pl.BlockSpec((1, 1, rows, rank), lambda i: (0, i, 0, 0)),
            pl.BlockSpec((1, 1, rows, rank), lambda i: (1, i, 0, 0)),
            pl.BlockSpec((1,) + w_in.shape, lambda i: (i, 0, 0)),
            pl.BlockSpec((1,) + w_out.shape, lambda i: (i, 0, 0)),
            fixed(dall),
        ],
        out_specs=tuple(
            spec or pl.BlockSpec(shape, lambda i, n=len(shape): (0,) * n) for shape, _, spec in outs
        ),
        scratch_shapes=[pltpu.VMEM((cols, rank), bf)],
        compiler_params=pltpu.CompilerParams(vmem_limit_bytes=VMEM_LIMIT),
        name="apply_step",
    )(*keep, ball, ball, win_all, wout_all, dall)


def solution(mesh):
    split, both = P("fs", None), P("fs", "tp")
    return jax.shard_map(
        functools.partial(shards, mesh),
        mesh=mesh,
        in_specs=(split, both, both, split, split, split, both, P("tp", "fs"), both, both, both, both),
        out_specs=(both, both, P(None, "tp"), both, both, P("tp", "fs"), P("tp", "fs"), P("tp", None), both, both),
        check_vma=False,
    )
```
